32 devices in a mesh: rep: 2 (over x), fs: 4 (over z), tp: 4 (over y, core).
Axes of the slice: x: 2, y: 2, z: 4, core: 2. Of those that a mesh axis runs over, the one named last changes fastest.
Arguments:
- tokens: bfloat16 [4096, 1024], P(('rep', 'fs', 'tp')), may hold values from -6 to 6
- w_up: bfloat16 [1024, 4096], P('fs', 'tp'), may hold values from -0.1875 to 0.1875
- w_down: bfloat16 [4096, 1024], P('tp', 'fs'), may hold values from -0.09375 to 0.09375
- out_gain: float32 [1024], replicated, may hold values from 0.1 to 1.9
- out_shift: float32 [1024], replicated, may hold values from -3 to 3
Outputs:
- normed: bfloat16 [4096, 1024], P(('rep', 'fs', 'tp'))
The draws below stay inside these ranges and needn't reach their ends.
All inputs are finite; a program needn't handle non-finite values.
Results may differ from the reference program's by a relative error of at most 0.015.
Values may be sent and summed in bfloat16 or wider, within the bound.
A program may use at most 64 MiB of HBM per device.

```python
import jax
import jax.numpy as jnp
from jax import lax

D = 1024
FF = 4096
TOKENS = 4096


def block_levels(rng, shape, split, low, high):
    gain, own = 1.0, jax.random.fold_in(rng, 6)
    for dim, blocks in split:
        heights = jnp.exp(jax.random.uniform(jax.random.fold_in(own, dim), (blocks,), jnp.float32, low / len(split), high / len(split)))
        gain = gain * jnp.repeat(heights, shape[dim] // blocks).reshape([-1 if axis == dim else 1 for axis in range(len(shape))])
    return gain


def scatter_about(key, shape, deviation, bound, pieces=(), held_as=jnp.bfloat16):
    values = jax.random.normal(key, shape, jnp.float32) * deviation
    if len(pieces) > 0:
        values = block_levels(key, shape, pieces, -0.22, 0.18) * values
    return jnp.clip(values, min=-bound, max=bound).astype(held_as)


def setup_inputs(seed: int = 0) -> dict:
    key_of = jax.random.split(jax.random.key(seed), 6)
    tokens = scatter_about(key_of[0], (TOKENS, D), 1.0, 6.0, ((0, 32),))
    w_up = scatter_about(key_of[1], (D, FF), D ** -0.5, 0.1875, ((0, 4), (1, 4)))
    w_down = scatter_about(key_of[2], (FF, D), FF ** -0.5, 0.09375, ((0, 4), (1, 4)))
    out_gain = jnp.clip(1.0 + 0.18 * jax.random.normal(key_of[3], (D,), jnp.float32), 0.1, 1.9)
    out_shift = scatter_about(key_of[4], (D,), 0.5, 3.0, (), jnp.float32)
    return dict(tokens=tokens, w_up=w_up, w_down=w_down, out_gain=out_gain, out_shift=out_shift)


residual_scale = 2.0 ** 0.25
norm_eps = 1e-05

def layer_norm(summed, out_gain, out_shift):
    row_mean = lax.optimization_barrier(jnp.mean(summed, axis=-1, keepdims=True))
    centered = summed - row_mean
    row_var = lax.optimization_barrier(jnp.mean(centered * centered, axis=-1, keepdims=True))
    return centered * lax.rsqrt(row_var + norm_eps) * out_gain + out_shift

def reference(tokens, w_up, w_down, out_gain, out_shift):
    pre_act = jnp.dot(tokens, w_up, preferred_element_type=jnp.float32)
    hidden = jnp.square(jnp.maximum(pre_act, 0.0)).astype(jnp.bfloat16)
    branch = jnp.dot(hidden, w_down, preferred_element_type=jnp.float32)
    summed = residual_scale * tokens.astype(jnp.float32) + branch
    return layer_norm(summed, out_gain, out_shift).astype(jnp.bfloat16)
```

```python
import functools

import jax
import jax.numpy as jnp
from jax import lax
from jax.experimental import pallas as pl
from jax.experimental.pallas import tpu as pltpu
from jax.sharding import PartitionSpec as P

residual_scale = 2.0**0.25
norm_eps = 1e-05


def kernel(
    sizes,
    tokens_ref, up_ref, down_ref, gain_ref, shift_ref,
    out_ref,
    tok, up, down, hidden, s1, r1, acc, s2, r2, own2,
    load_sem, tok_send, tok_recv, fwd_send, up_send, up_recv,
    down_send, down_recv, s1_send, r1_recv, s2_send, r2_recv,
):
    R, F, T = sizes
    Y = T // 2
    pairs = R * Y
    own = tokens_ref.shape[0]
    H = up.shape[2]
    half = H // 2
    Dc = down.shape[2]
    r, f, t = lax.axis_index("rep"), lax.axis_index("fs"), lax.axis_index("tp")
    y, c = t // 2, t % 2
    q = r * Y + y
    mine = c * pairs + q

    def dev(rr, ff, tt):
        return {"rep": rr, "fs": ff, "tp": tt}

    partner = dev(r, f, y * 2 + (1 - c))
    peers = []
    for dr in range(R):
        for dy in range(Y):
            if dr or dy:
                rr, yy = (r + dr) % R, (y + dy) % Y
                sr, sy = (r + R - dr) % R, (y + Y - dy) % Y
                peers.append((dev(rr, f, yy * 2 + c), rr * Y + yy, sr * Y + sy))

    def remote(src, dst, ss, rs, device):
        return pltpu.make_async_remote_copy(
            src_ref=src, dst_ref=dst, send_sem=ss, recv_sem=rs,
            device_id=device, device_id_type=pl.DeviceIdType.MESH,
        )

    base = pl.multiple_of(r * H, H)
    loads = [
        pltpu.make_async_copy(up_ref.at[:, pl.ds(base, H)], up.at[f], load_sem.at[0]),
        pltpu.make_async_copy(tokens_ref, tok.at[mine], load_sem.at[1]),
        pltpu.make_async_copy(down_ref.at[pl.ds(base, H), :], down.at[f], load_sem.at[2]),
    ]
    for load in loads:
        load.start()

    barrier = pltpu.get_barrier_semaphore()

    def greet(device):
        pl.semaphore_signal(barrier, inc=1, device_id=device, device_id_type=pl.DeviceIdType.MESH)

    greet(partner)
    for device, _, _ in peers:
        greet(device)

    @pl.when(f > 0)
    def _():
        greet(dev(r, f - 1, t))

    @pl.when(f < F - 1)
    def _():
        greet(dev(r, f + 1, t))

    neighbours = jnp.where(f > 0, 1, 0) + jnp.where(f < F - 1, 1, 0)
    pl.semaphore_wait(barrier, 1 + len(peers) + neighbours)

    def up_copy(piece, to, n):
        return remote(up.at[piece], up.at[piece], up_send.at[n], up_recv.at[piece], dev(r, to, t))

    def down_copy(piece, part, to, n):
        block = down.at[piece, pl.ds(part * half, half)]
        return remote(block, block, down_send.at[n, part], down_recv.at[piece, part], dev(r, to, t))

    def guarded(condition, action):
        @pl.when(condition)
        def _():
            action()

    last = 2 * F - 2

    def own_sends(copy):
        guarded(f < F - 1, lambda: copy(f + 1, last + 1).start())
        guarded(f > 0, lambda: copy(f - 1, 0).start())

    loads[0].wait()
    own_sends(lambda to, n: up_copy(f, to, n))
    loads[1].wait()
    tok_copies = [remote(tok.at[mine], tok.at[mine], tok_send.at[0], tok_recv.at[mine], partner)]
    for k, (device, _, _) in enumerate(peers):
        tok_copies.append(remote(tok.at[mine], tok.at[mine], tok_send.at[k + 1], tok_recv.at[mine], device))
    for copy in tok_copies[1:] + tok_copies[:1]:
        copy.start()
    loads[2].wait()
    own_sends(lambda to, n: down_copy(f, 0, to, n))

    def up_visit(v):
        s = (v - 1) // 2
        if v % 2:
            piece, to = f - 1 - s, f + 1
            here, onward = piece >= 0, jnp.logical_and(piece >= 0, f < F - 1)
        else:
            piece, to = f + 1 + s, f - 1
            here, onward = piece < F, jnp.logical_and(piece < F, f > 0)
        return piece, to, here, onward

    def take_up(v):
        piece, to, here, onward = up_visit(v)
        guarded(here, lambda: up_copy(piece, f, v).wait_recv())
        guarded(onward, lambda: up_copy(piece, to, v).start())

    for v in (1, 2):
        if v <= last:
            take_up(v)
    own_sends(lambda to, n: down_copy(f, 1, to, n))

    fwd_copies = []
    for k, (_, _, source) in enumerate(peers):
        slot = c * pairs + source
        remote(tok.at[slot], tok.at[slot], tok_send.at[0], tok_recv.at[slot], partner).wait_recv()
        fwd = remote(tok.at[slot], tok.at[slot], fwd_send.at[k], tok_recv.at[slot], partner)
        fwd.start()
        fwd_copies.append(fwd)

    for v in range(3, last + 1):
        take_up(v)
    for k in range(pairs):
        slot = (1 - c) * pairs + k
        remote(tok.at[slot], tok.at[slot], tok_send.at[0], tok_recv.at[slot], partner).wait_recv()

    rows = pairs * own
    chunk = 2 if pairs % 2 == 0 else 1
    weights = lambda: up[...].reshape(up.shape[0] * up.shape[1], H)

    @pl.loop(0, 2 * pairs // chunk)
    def _(n):
        block = tok[pl.ds(n * chunk, chunk)].reshape(chunk * own, tok.shape[2])
        pre_act = jnp.dot(block, weights(), preferred_element_type=jnp.float32)
        kept = jnp.square(jnp.maximum(pre_act, 0.0)).astype(jnp.bfloat16)
        hidden[pl.ds(pl.multiple_of(n * chunk * own, chunk * own), chunk * own), :] = kept

    def half_product(side, piece):
        picked = hidden[pl.ds(pl.multiple_of(side * rows, rows), rows), :]
        product = jnp.dot(picked, down[piece], preferred_element_type=jnp.float32)
        return product.reshape(pairs, own, Dc)

    def project(piece):
        s1[piece] = half_product(1 - c, piece).astype(jnp.bfloat16)
        swap = remote(s1.at[piece], r1.at[piece], s1_send.at[piece], r1_recv.at[piece], partner)
        swap.start()
        acc[...] = half_product(c, piece)
        swap.wait_recv()
        for k, (device, target, _) in enumerate(peers):
            s2[piece, k] = (acc[target] + r1[piece, target].astype(jnp.float32)).astype(jnp.bfloat16)
            remote(s2.at[piece, k], r2.at[piece, k], s2_send.at[piece], r2_recv.at[piece], device).start()
        own2[piece] = acc[q] + r1[piece, q].astype(jnp.float32)

    def visit(v):
        s = (v - 1) // 2
        odd = v % 2 == 1
        piece = jnp.where(v == 0, f, jnp.where(odd, f - 1 - s, f + 1 + s))
        to = jnp.where(odd, f + 1, f - 1)
        here = jnp.logical_and(piece >= 0, piece < F)
        onward = jnp.logical_and(jnp.logical_and(here, v > 0), jnp.logical_and(to >= 0, to < F))
        return piece, to, here, onward

    @pl.loop(0, last + 1)
    def _(v):
        piece, to, here, onward = visit(v)

        @pl.when(jnp.logical_and(here, v > 0))
        def _():
            for part in range(2):
                down_copy(piece, part, f, v).wait_recv()

                @pl.when(onward)
                def _():
                    down_copy(piece, part, to, v).start()

        @pl.when(here)
        def _():
            project(piece)

    for piece in range(F):
        pltpu.make_async_copy(r2.at[piece], r2.at[piece], r2_recv.at[piece]).wait()

    summed = []
    for piece in range(F):
        part = residual_scale * tok[mine, :, piece * Dc:(piece + 1) * Dc].astype(jnp.float32) + own2[piece]
        for k in range(len(peers)):
            part = part + r2[piece, k].astype(jnp.float32)
        summed.append(part)
    width = F * Dc
    row_mean = functools.reduce(jnp.add, [jnp.sum(p, axis=-1, keepdims=True) for p in summed]) / width
    centered = [p - row_mean for p in summed]
    row_var = functools.reduce(jnp.add, [jnp.sum(p * p, axis=-1, keepdims=True) for p in centered]) / width
    inverse = lax.rsqrt(row_var + norm_eps)
    for piece in range(F):
        cols = slice(piece * Dc, (piece + 1) * Dc)
        out_ref[:, cols] = (centered[piece] * inverse * gain_ref[:, cols] + shift_ref[:, cols]).astype(out_ref.dtype)

    own_sends_done = lambda copy: (
        guarded(f < F - 1, lambda: copy(f + 1, last + 1).wait_send()),
        guarded(f > 0, lambda: copy(f - 1, 0).wait_send()),
    )
    own_sends_done(lambda to, n: up_copy(f, to, n))
    for part in range(2):
        own_sends_done(lambda to, n: down_copy(f, part, to, n))
    for copy in tok_copies + fwd_copies:
        copy.wait_send()
    for v in range(1, last + 1):
        piece, to, here, onward = up_visit(v)
        guarded(onward, lambda: up_copy(piece, to, v).wait_send())
        for part in range(2):
            guarded(onward, lambda: down_copy(piece, part, to, v).wait_send())
    for piece in range(F):
        remote(s1.at[piece], r1.at[piece], s1_send.at[piece], r1_recv.at[piece], partner).wait_send()
        pltpu.make_async_copy(s2.at[piece], s2.at[piece], s2_send.at[piece]).wait()


def shards(sizes, tokens, w_up, w_down, out_gain, out_shift):
    R, F, T = sizes
    pairs = R * T // 2
    group = R * T
    own, D = tokens.shape
    H = w_up.shape[1] // R
    Dc = w_down.shape[1]
    others = pairs - 1
    visits = 2 * F
    dma = pltpu.SemaphoreType.DMA
    whole = pl.BlockSpec(memory_space=pltpu.VMEM)
    anywhere = pl.BlockSpec(memory_space=pl.ANY)
    return pl.pallas_call(
        functools.partial(kernel, sizes),
        out_shape=jax.ShapeDtypeStruct((own, D), jnp.bfloat16),
        in_specs=[anywhere, anywhere, anywhere, whole, whole],
        out_specs=whole,
        scratch_shapes=[
            pltpu.VMEM((group, own, D), jnp.bfloat16),
            pltpu.VMEM((F, D // F, H), jnp.bfloat16),
            pltpu.VMEM((F, H, Dc), jnp.bfloat16),
            pltpu.VMEM((group * own, H), jnp.bfloat16),
            pltpu.VMEM((F, pairs, own, Dc), jnp.bfloat16),
            pltpu.VMEM((F, pairs, own, Dc), jnp.bfloat16),
            pltpu.VMEM((pairs, own, Dc), jnp.float32),
            pltpu.VMEM((F, others, own, Dc), jnp.bfloat16),
            pltpu.VMEM((F, others, own, Dc), jnp.bfloat16),
            pltpu.VMEM((F, own, Dc), jnp.float32),
            dma((3,)),
            dma((pairs,)),
            dma((group,)),
            dma((others,)),
            dma((visits,)),
            dma((F,)),
            dma((visits, 2)),
            dma((F, 2)),
            dma((F,)),
            dma((F,)),
            dma((F,)),
            dma((F,)),
        ],
        compiler_params=pltpu.CompilerParams(
            collective_id=0, has_side_effects=True, vmem_limit_bytes=48 * 1024 * 1024
        ),
        name="feed_forward",
    )(tokens, w_up, w_down, out_gain.reshape(1, D), out_shift.reshape(1, D))


def solution(mesh):
    sizes = (mesh.shape["rep"], mesh.shape["fs"], mesh.shape["tp"])
    in_specs = (P(("rep", "fs", "tp"), None), P("fs", "tp"), P("tp", "fs"), P(), P())
    out_specs = P(("rep", "fs", "tp"), None)
    return jax.shard_map(
        functools.partial(shards, sizes), mesh=mesh, in_specs=in_specs, out_specs=out_specs, check_vma=False
    )
```

```python
import functools

import jax
import jax.numpy as jnp
from jax import lax
from jax.experimental import pallas as pl
from jax.experimental.pallas import tpu as pltpu
from jax.sharding import PartitionSpec as P

residual_scale = 2.0**0.25
norm_eps = 1e-05


def kernel(
    sizes,
    tokens_ref, up_ref, down_ref, gain_ref, shift_ref,
    out_ref,
    tok, up, down, gain, shift, hidden, s1, r1, acc, s2, r2, own2,
    load_sem, tok_send, tok_recv, fwd_send, up_send, up_recv,
    down_send, down_recv, s1_send, r1_recv, s2_send, r2_recv,
):
    R, F, T = sizes
    Y = T // 2
    pairs = R * Y
    own = tokens_ref.shape[0]
    H = up.shape[2]
    parts = down.shape[0] // F
    Dp = down.shape[2]
    r, f, t = lax.axis_index("rep"), lax.axis_index("fs"), lax.axis_index("tp")
    y, c = t // 2, t % 2
    q = r * Y + y
    mine = c * pairs + q

    def dev(rr, ff, tt):
        return {"rep": rr, "fs": ff, "tp": tt}

    partner = dev(r, f, y * 2 + (1 - c))
    peers = []
    for dr in range(R):
        for dy in range(Y):
            if dr or dy:
                rr, yy = (r + dr) % R, (y + dy) % Y
                sr, sy = (r + R - dr) % R, (y + Y - dy) % Y
                peers.append((dev(rr, f, yy * 2 + c), rr * Y + yy, sr * Y + sy))

    def remote(src, dst, ss, rs, device):
        return pltpu.make_async_remote_copy(
            src_ref=src, dst_ref=dst, send_sem=ss, recv_sem=rs,
            device_id=device, device_id_type=pl.DeviceIdType.MESH,
        )

    base = pl.multiple_of(r * H, H)
    loads = [
        pltpu.make_async_copy(up_ref.at[:, pl.ds(base, H)], up.at[f], load_sem.at[0]),
        pltpu.make_async_copy(tokens_ref, tok.at[mine], load_sem.at[1]),
        pltpu.make_async_copy(gain_ref, gain, load_sem.at[2]),
        pltpu.make_async_copy(shift_ref, shift, load_sem.at[3]),
    ]
    for part in range(parts):
        block = down_ref.at[pl.ds(base, H), pl.ds(part * Dp, Dp)]
        loads.append(pltpu.make_async_copy(block, down.at[f * parts + part], load_sem.at[4 + part]))
    for load in loads:
        load.start()

    barrier = pltpu.get_barrier_semaphore()

    def greet(device):
        pl.semaphore_signal(barrier, inc=1, device_id=device, device_id_type=pl.DeviceIdType.MESH)

    greet(partner)
    for device, _, _ in peers:
        greet(device)

    @pl.when(f > 0)
    def _():
        greet(dev(r, f - 1, t))

    @pl.when(f < F - 1)
    def _():
        greet(dev(r, f + 1, t))

    neighbours = jnp.where(f > 0, 1, 0) + jnp.where(f < F - 1, 1, 0)
    pl.semaphore_wait(barrier, 1 + len(peers) + neighbours)

    def up_copy(piece, to, n):
        return remote(up.at[piece], up.at[piece], up_send.at[n], up_recv.at[piece], dev(r, to, t))

    def down_copy(piece, part, to, n):
        block = down.at[piece * parts + part]
        return remote(block, block, down_send.at[n, part], down_recv.at[piece, part], dev(r, to, t))

    def guarded(condition, action):
        @pl.when(condition)
        def _():
            action()

    last = 2 * F - 2

    def own_sends(copy):
        guarded(f < F - 1, lambda: copy(f + 1, last + 1).start())
        guarded(f > 0, lambda: copy(f - 1, 0).start())

    loads[0].wait()
    own_sends(lambda to, n: up_copy(f, to, n))
    loads[1].wait()
    tok_copies = [remote(tok.at[mine], tok.at[mine], tok_send.at[0], tok_recv.at[mine], partner)]
    for k, (device, _, _) in enumerate(peers):
        tok_copies.append(remote(tok.at[mine], tok.at[mine], tok_send.at[k + 1], tok_recv.at[mine], device))
    for copy in tok_copies[1:] + tok_copies[:1]:
        copy.start()
    for load in loads[2:]:
        load.wait()
    own_sends(lambda to, n: down_copy(f, 0, to, n))

    def up_visit(v):
        s = (v - 1) // 2
        if v % 2:
            piece, to = f - 1 - s, f + 1
            here, onward = piece >= 0, jnp.logical_and(piece >= 0, f < F - 1)
        else:
            piece, to = f + 1 + s, f - 1
            here, onward = piece < F, jnp.logical_and(piece < F, f > 0)
        return piece, to, here, onward

    def take_up(v):
        piece, to, here, onward = up_visit(v)
        guarded(here, lambda: up_copy(piece, f, v).wait_recv())
        guarded(onward, lambda: up_copy(piece, to, v).start())

    for v in (1, 2):
        if v <= last:
            take_up(v)
    for part in range(1, parts):
        own_sends(lambda to, n: down_copy(f, part, to, n))

    fwd_copies = []
    for k, (_, _, source) in enumerate(peers):
        slot = c * pairs + source
        remote(tok.at[slot], tok.at[slot], tok_send.at[0], tok_recv.at[slot], partner).wait_recv()
        fwd = remote(tok.at[slot], tok.at[slot], fwd_send.at[k], tok_recv.at[slot], partner)
        fwd.start()
        fwd_copies.append(fwd)

    for v in range(3, last + 1):
        take_up(v)
    for k in range(pairs):
        slot = (1 - c) * pairs + k
        remote(tok.at[slot], tok.at[slot], tok_send.at[0], tok_recv.at[slot], partner).wait_recv()

    def visit(v):
        step = (v - 1) // 2
        odd = v % 2 == 1
        piece = jnp.where(odd, f - 1 - step, f + 1 + step)
        to = jnp.where(odd, f + 1, f - 1)
        here = jnp.logical_and(v <= last, jnp.logical_and(piece >= 0, piece < F))
        passes = jnp.logical_and(to >= 0, to < F)
        return piece, to, jnp.logical_and(here, passes), jnp.logical_and(here, jnp.logical_not(passes))

    def pass_down(v):
        piece, to, onward, _ = visit(v)

        @pl.when(onward)
        def _():
            for part in range(parts):
                down_copy(piece, part, f, v).wait_recv()
                down_copy(piece, part, to, v).start()

    for v in (1, 2):
        if v <= last:
            pass_down(v)

    rows = pairs * own
    chunk = 2 if pairs % 2 == 0 else 1
    weights = lambda: up[...].reshape(up.shape[0] * up.shape[1], H)

    @pl.loop(0, 2 * pairs // chunk)
    def _(n):
        block = tok[pl.ds(n * chunk, chunk)].reshape(chunk * own, tok.shape[2])
        pre_act = jnp.dot(block, weights(), preferred_element_type=jnp.float32)
        kept = jnp.square(jnp.maximum(pre_act, 0.0)).astype(jnp.bfloat16)
        hidden[pl.ds(pl.multiple_of(n * chunk * own, chunk * own), chunk * own), :] = kept

    def half_product(side, block):
        picked = hidden[pl.ds(pl.multiple_of(side * rows, rows), rows), :]
        product = jnp.dot(picked, down[block], preferred_element_type=jnp.float32)
        return product.reshape(pairs, own, Dp)

    def project(block):
        s1[block] = half_product(1 - c, block).astype(jnp.bfloat16)
        swap = remote(s1.at[block], r1.at[block], s1_send.at[block], r1_recv.at[block], partner)
        swap.start()
        acc[...] = half_product(c, block)
        swap.wait_recv()
        for k, (device, target, _) in enumerate(peers):
            s2[block, k] = (acc[target] + r1[block, target].astype(jnp.float32)).astype(jnp.bfloat16)
            remote(s2.at[block, k], r2.at[block, k], s2_send.at[block], r2_recv.at[block], device).start()
        own2[block] = acc[q] + r1[block, q].astype(jnp.float32)

    @pl.loop(0, F)
    def _(step):
        @pl.when(step > 0)
        def _():
            pass_down(2 * step + 1)
            pass_down(2 * step + 2)

        @pl.loop(0, 2 * parts)
        def _(n):
            part = n % parts
            v = 2 * step - 1 + n // parts
            piece, _, onward, ends = visit(v)
            piece = jnp.where(step == 0, f, piece)
            remote_here = jnp.logical_and(step > 0, jnp.logical_or(onward, ends))

            @pl.when(jnp.logical_and(step > 0, ends))
            def _():
                down_copy(piece, part, f, 0).wait_recv()

            @pl.when(jnp.logical_or(remote_here, jnp.logical_and(step == 0, n < parts)))
            def _():
                project(piece * parts + part)

    blocks = F * parts
    for block in range(blocks):
        pltpu.make_async_copy(r2.at[block], r2.at[block], r2_recv.at[block]).wait()

    summed = []
    for block in range(blocks):
        term = residual_scale * tok[mine, :, block * Dp:(block + 1) * Dp].astype(jnp.float32) + own2[block]
        for k in range(len(peers)):
            term = term + r2[block, k].astype(jnp.float32)
        summed.append(term)
    width = blocks * Dp
    row_mean = functools.reduce(jnp.add, [jnp.sum(p, axis=-1, keepdims=True) for p in summed]) / width
    centered = [p - row_mean for p in summed]
    row_var = functools.reduce(jnp.add, [jnp.sum(p * p, axis=-1, keepdims=True) for p in centered]) / width
    inverse = lax.rsqrt(row_var + norm_eps)
    for block in range(blocks):
        cols = slice(block * Dp, (block + 1) * Dp)
        out_ref[:, cols] = (centered[block] * inverse * gain[:, cols] + shift[:, cols]).astype(out_ref.dtype)

    own_sends_done = lambda copy: (
        guarded(f < F - 1, lambda: copy(f + 1, last + 1).wait_send()),
        guarded(f > 0, lambda: copy(f - 1, 0).wait_send()),
    )
    own_sends_done(lambda to, n: up_copy(f, to, n))
    for part in range(parts):
        own_sends_done(lambda to, n: down_copy(f, part, to, n))
    for copy in tok_copies + fwd_copies:
        copy.wait_send()
    for v in range(1, last + 1):
        piece, to, here, onward = up_visit(v)
        guarded(onward, lambda: up_copy(piece, to, v).wait_send())
        for part in range(parts):
            guarded(onward, lambda: down_copy(piece, part, to, v).wait_send())
    for block in range(blocks):
        remote(s1.at[block], r1.at[block], s1_send.at[block], r1_recv.at[block], partner).wait_send()
        pltpu.make_async_copy(s2.at[block], s2.at[block], s2_send.at[block]).wait()


def shards(sizes, tokens, w_up, w_down, out_gain, out_shift):
    R, F, T = sizes
    pairs = R * T // 2
    group = R * T
    own, D = tokens.shape
    H = w_up.shape[1] // R
    Dc = w_down.shape[1]
    others = pairs - 1
    visits = 2 * F
    parts = 2 if Dc % 256 == 0 else 1
    blocks, Dp = F * parts, Dc // parts
    dma = pltpu.SemaphoreType.DMA
    whole = pl.BlockSpec(memory_space=pltpu.VMEM)
    in_hbm = pl.BlockSpec(memory_space=pltpu.HBM)
    return pl.pallas_call(
        functools.partial(kernel, sizes),
        out_shape=jax.ShapeDtypeStruct((own, D), jnp.bfloat16),
        in_specs=[in_hbm] * 5,
        out_specs=whole,
        scratch_shapes=[
            pltpu.VMEM((group, own, D), jnp.bfloat16),
            pltpu.VMEM((F, D // F, H), jnp.bfloat16),
            pltpu.VMEM((blocks, H, Dp), jnp.bfloat16),
            pltpu.VMEM((1, D), jnp.float32),
            pltpu.VMEM((1, D), jnp.float32),
            pltpu.VMEM((group * own, H), jnp.bfloat16),
            pltpu.VMEM((blocks, pairs, own, Dp), jnp.bfloat16),
            pltpu.VMEM((blocks, pairs, own, Dp), jnp.bfloat16),
            pltpu.VMEM((pairs, own, Dp), jnp.float32),
            pltpu.VMEM((blocks, others, own, Dp), jnp.bfloat16),
            pltpu.VMEM((blocks, others, own, Dp), jnp.bfloat16),
            pltpu.VMEM((blocks, own, Dp), jnp.float32),
            dma((4 + parts,)),
            dma((pairs,)),
            dma((group,)),
            dma((others,)),
            dma((visits,)),
            dma((F,)),
            dma((visits, parts)),
            dma((F, parts)),
            dma((blocks,)),
            dma((blocks,)),
            dma((blocks,)),
            dma((blocks,)),
        ],
        compiler_params=pltpu.CompilerParams(
            collective_id=0, has_side_effects=True, vmem_limit_bytes=67_043_328
        ),
        name="feed_forward",
    )(tokens, w_up, w_down, out_gain.reshape(1, D), out_shift.reshape(1, D))


def solution(mesh):
    sizes = (mesh.shape["rep"], mesh.shape["fs"], mesh.shape["tp"])
    in_specs = (P(("rep", "fs", "tp"), None), P("fs", "tp"), P("tp", "fs"), P(), P())
    out_specs = P(("rep", "fs", "tp"), None)
    return jax.shard_map(
        functools.partial(shards, sizes), mesh=mesh, in_specs=in_specs, out_specs=out_specs, check_vma=False
    )
```

```python
import functools

import jax
import jax.numpy as jnp
from jax import lax
from jax.experimental import pallas as pl
from jax.experimental.pallas import tpu as pltpu
from jax.sharding import PartitionSpec as P

residual_scale = 2.0**0.25
norm_eps = 1e-05


def kernel(
    sizes,
    tokens_ref, up_ref, down_ref, gain_ref, shift_ref,
    out_ref,
    tok, up, down, gain, shift, hidden, s1, r1, acc, s2, r2, own2,
    load_sem, tok_send, tok_recv, fwd_send, up_send, up_recv,
    down_send, down_recv, s1_send, r1_recv, s2_send, r2_recv,
):
    R, F, T = sizes
    Y = T // 2
    pairs = R * Y
    own = tokens_ref.shape[0]
    H = up.shape[2]
    parts = down.shape[0] // F
    Dp = down.shape[2]
    r, f, t = lax.axis_index("rep"), lax.axis_index("fs"), lax.axis_index("tp")
    y, c = t // 2, t % 2
    q = r * Y + y
    mine = c * pairs + q

    def dev(rr, ff, tt):
        return {"rep": rr, "fs": ff, "tp": tt}

    partner = dev(r, f, y * 2 + (1 - c))
    peers = []
    for dr in range(R):
        for dy in range(Y):
            if dr or dy:
                rr, yy = (r + dr) % R, (y + dy) % Y
                sr, sy = (r + R - dr) % R, (y + Y - dy) % Y
                peers.append((dev(rr, f, yy * 2 + c), rr * Y + yy, sr * Y + sy))

    def remote(src, dst, ss, rs, device):
        return pltpu.make_async_remote_copy(
            src_ref=src, dst_ref=dst, send_sem=ss, recv_sem=rs,
            device_id=device, device_id_type=pl.DeviceIdType.MESH,
        )

    base = pl.multiple_of(r * H, H)
    loads = [
        pltpu.make_async_copy(up_ref.at[:, pl.ds(base, H)], up.at[f], load_sem.at[0]),
        pltpu.make_async_copy(tokens_ref, tok.at[mine], load_sem.at[1]),
        pltpu.make_async_copy(gain_ref, gain, load_sem.at[2]),
        pltpu.make_async_copy(shift_ref, shift, load_sem.at[3]),
    ]
    for part in range(parts):
        block = down_ref.at[pl.ds(base, H), pl.ds(part * Dp, Dp)]
        loads.append(pltpu.make_async_copy(block, down.at[f * parts + part], load_sem.at[4 + part]))
    for load in loads:
        load.start()

    barrier = pltpu.get_barrier_semaphore()

    def greet(device):
        pl.semaphore_signal(barrier, inc=1, device_id=device, device_id_type=pl.DeviceIdType.MESH)

    greet(partner)
    for device, _, _ in peers:
        greet(device)

    @pl.when(f > 0)
    def _():
        greet(dev(r, f - 1, t))

    @pl.when(f < F - 1)
    def _():
        greet(dev(r, f + 1, t))

    neighbours = jnp.where(f > 0, 1, 0) + jnp.where(f < F - 1, 1, 0)
    pl.semaphore_wait(barrier, 1 + len(peers) + neighbours)

    def up_copy(piece, to, n):
        return remote(up.at[piece], up.at[piece], up_send.at[n], up_recv.at[piece], dev(r, to, t))

    def down_copy(piece, part, to, n):
        block = down.at[piece * parts + part]
        return remote(block, block, down_send.at[n, part], down_recv.at[piece, part], dev(r, to, t))

    def guarded(condition, action):
        @pl.when(condition)
        def _():
            action()

    last = 2 * F - 2

    def own_sends(copy):
        guarded(f < F - 1, lambda: copy(f + 1, last + 1).start())
        guarded(f > 0, lambda: copy(f - 1, 0).start())

    loads[0].wait()
    own_sends(lambda to, n: up_copy(f, to, n))
    loads[1].wait()
    tok_copies = [remote(tok.at[mine], tok.at[mine], tok_send.at[0], tok_recv.at[mine], partner)]
    for k, (device, _, _) in enumerate(peers):
        tok_copies.append(remote(tok.at[mine], tok.at[mine], tok_send.at[k + 1], tok_recv.at[mine], device))
    for copy in tok_copies[1:] + tok_copies[:1]:
        copy.start()
    for load in loads[2:]:
        load.wait()
    own_sends(lambda to, n: down_copy(f, 0, to, n))

    def up_visit(v):
        s = (v - 1) // 2
        if v % 2:
            piece, to = f - 1 - s, f + 1
            here, onward = piece >= 0, jnp.logical_and(piece >= 0, f < F - 1)
        else:
            piece, to = f + 1 + s, f - 1
            here, onward = piece < F, jnp.logical_and(piece < F, f > 0)
        return piece, to, here, onward

    def take_up(v):
        piece, to, here, onward = up_visit(v)
        guarded(here, lambda: up_copy(piece, f, v).wait_recv())
        guarded(onward, lambda: up_copy(piece, to, v).start())

    for v in (1, 2):
        if v <= last:
            take_up(v)
    for part in range(1, parts):
        own_sends(lambda to, n: down_copy(f, part, to, n))

    def visit(v):
        step = (v - 1) // 2
        odd = v % 2 == 1
        piece = jnp.where(odd, f - 1 - step, f + 1 + step)
        to = jnp.where(odd, f + 1, f - 1)
        here = jnp.logical_and(v <= last, jnp.logical_and(piece >= 0, piece < F))
        passes = jnp.logical_and(to >= 0, to < F)
        return piece, to, jnp.logical_and(here, passes), jnp.logical_and(here, jnp.logical_not(passes))

    def pass_down(v, only=None):
        piece, to, onward, _ = visit(v)
        if only is not None:
            onward = jnp.logical_and(onward, only(piece))

        @pl.when(onward)
        def _():
            for part in range(parts):
                down_copy(piece, part, f, v).wait_recv()
                down_copy(piece, part, to, v).start()

    def from_end(piece):
        return jnp.logical_or(piece == 0, piece == F - 1)

    for v in (1, 2):
        if v <= last:
            pass_down(v, from_end)

    fwd_copies = []
    for k, (_, _, source) in enumerate(peers):
        slot = c * pairs + source
        remote(tok.at[slot], tok.at[slot], tok_send.at[0], tok_recv.at[slot], partner).wait_recv()
        fwd = remote(tok.at[slot], tok.at[slot], fwd_send.at[k], tok_recv.at[slot], partner)
        fwd.start()
        fwd_copies.append(fwd)

    for v in range(3, last + 1):
        take_up(v)
    for k in range(pairs):
        slot = (1 - c) * pairs + k
        remote(tok.at[slot], tok.at[slot], tok_send.at[0], tok_recv.at[slot], partner).wait_recv()

    for v in (1, 2):
        if v <= last:
            pass_down(v, lambda piece: jnp.logical_not(from_end(piece)))

    rows = pairs * own
    chunk = 2 if pairs % 2 == 0 else 1
    weights = lambda: up[...].reshape(up.shape[0] * up.shape[1], H)

    @pl.loop(0, 2 * pairs // chunk)
    def _(n):
        block = tok[pl.ds(n * chunk, chunk)].reshape(chunk * own, tok.shape[2])
        pre_act = jnp.dot(block, weights(), preferred_element_type=jnp.float32)
        kept = jnp.square(jnp.maximum(pre_act, 0.0)).astype(jnp.bfloat16)
        hidden[pl.ds(pl.multiple_of(n * chunk * own, chunk * own), chunk * own), :] = kept

    def half_product(side, block):
        picked = hidden[pl.ds(pl.multiple_of(side * rows, rows), rows), :]
        product = jnp.dot(picked, down[block], preferred_element_type=jnp.float32)
        return product.reshape(pairs, own, Dp)

    def project(block):
        s1[block] = half_product(1 - c, block).astype(jnp.bfloat16)
        swap = remote(s1.at[block], r1.at[block], s1_send.at[block], r1_recv.at[block], partner)
        swap.start()
        acc[...] = half_product(c, block)
        swap.wait_recv()
        for k, (device, target, _) in enumerate(peers):
            s2[block, k] = (acc[target] + r1[block, target].astype(jnp.float32)).astype(jnp.bfloat16)
            remote(s2.at[block, k], r2.at[block, k], s2_send.at[block], r2_recv.at[block], device).start()
        own2[block] = acc[q] + r1[block, q].astype(jnp.float32)

    @pl.loop(0, F)
    def _(step):
        pass_down(2 * step + 3)
        pass_down(2 * step + 4)

        @pl.loop(0, 2 * parts)
        def _(n):
            part = n % parts
            v = 2 * step - 1 + n // parts
            piece, _, onward, ends = visit(v)
            piece = jnp.where(step == 0, f, piece)
            remote_here = jnp.logical_and(step > 0, jnp.logical_or(onward, ends))

            @pl.when(jnp.logical_and(step > 0, ends))
            def _():
                down_copy(piece, part, f, 0).wait_recv()

            @pl.when(jnp.logical_or(remote_here, jnp.logical_and(step == 0, n < parts)))
            def _():
                project(piece * parts + part)

    blocks = F * parts
    for block in range(blocks):
        pltpu.make_async_copy(r2.at[block], r2.at[block], r2_recv.at[block]).wait()

    summed = []
    for block in range(blocks):
        term = residual_scale * tok[mine, :, block * Dp:(block + 1) * Dp].astype(jnp.float32) + own2[block]
        for k in range(len(peers)):
            term = term + r2[block, k].astype(jnp.float32)
        summed.append(term)
    width = blocks * Dp
    row_mean = functools.reduce(jnp.add, [jnp.sum(p, axis=-1, keepdims=True) for p in summed]) / width
    centered = [p - row_mean for p in summed]
    row_var = functools.reduce(jnp.add, [jnp.sum(p * p, axis=-1, keepdims=True) for p in centered]) / width
    inverse = lax.rsqrt(row_var + norm_eps)
    for block in range(blocks):
        cols = slice(block * Dp, (block + 1) * Dp)
        out_ref[:, cols] = (centered[block] * inverse * gain[:, cols] + shift[:, cols]).astype(out_ref.dtype)

    own_sends_done = lambda copy: (
        guarded(f < F - 1, lambda: copy(f + 1, last + 1).wait_send()),
        guarded(f > 0, lambda: copy(f - 1, 0).wait_send()),
    )
    own_sends_done(lambda to, n: up_copy(f, to, n))
    for part in range(parts):
        own_sends_done(lambda to, n: down_copy(f, part, to, n))
    for copy in tok_copies + fwd_copies:
        copy.wait_send()
    for v in range(1, last + 1):
        piece, to, here, onward = up_visit(v)
        guarded(onward, lambda: up_copy(piece, to, v).wait_send())
        for part in range(parts):
            guarded(onward, lambda: down_copy(piece, part, to, v).wait_send())
    for block in range(blocks):
        remote(s1.at[block], r1.at[block], s1_send.at[block], r1_recv.at[block], partner).wait_send()
        pltpu.make_async_copy(s2.at[block], s2.at[block], s2_send.at[block]).wait()


def shards(sizes, tokens, w_up, w_down, out_gain, out_shift):
    R, F, T = sizes
    pairs = R * T // 2
    group = R * T
    own, D = tokens.shape
    H = w_up.shape[1] // R
    Dc = w_down.shape[1]
    others = pairs - 1
    visits = 2 * F
    parts = 2 if Dc % 256 == 0 else 1
    blocks, Dp = F * parts, Dc // parts
    dma = pltpu.SemaphoreType.DMA
    whole = pl.BlockSpec(memory_space=pltpu.VMEM)
    in_hbm = pl.BlockSpec(memory_space=pltpu.HBM)
    return pl.pallas_call(
        functools.partial(kernel, sizes),
        out_shape=jax.ShapeDtypeStruct((own, D), jnp.bfloat16),
        in_specs=[in_hbm] * 5,
        out_specs=whole,
        scratch_shapes=[
            pltpu.VMEM((group, own, D), jnp.bfloat16),
            pltpu.VMEM((F, D // F, H), jnp.bfloat16),
            pltpu.VMEM((blocks, H, Dp), jnp.bfloat16),
            pltpu.VMEM((1, D), jnp.float32),
            pltpu.VMEM((1, D), jnp.float32),
            pltpu.VMEM((group * own, H), jnp.bfloat16),
            pltpu.VMEM((blocks, pairs, own, Dp), jnp.bfloat16),
            pltpu.VMEM((blocks, pairs, own, Dp), jnp.bfloat16),
            pltpu.VMEM((pairs, own, Dp), jnp.float32),
            pltpu.VMEM((blocks, others, own, Dp), jnp.bfloat16),
            pltpu.VMEM((blocks, others, own, Dp), jnp.bfloat16),
            pltpu.VMEM((blocks, own, Dp), jnp.float32),
            dma((4 + parts,)),
            dma((pairs,)),
            dma((group,)),
            dma((others,)),
            dma((visits,)),
            dma((F,)),
            dma((visits, parts)),
            dma((F, parts)),
            dma((blocks,)),
            dma((blocks,)),
            dma((blocks,)),
            dma((blocks,)),
        ],
        compiler_params=pltpu.CompilerParams(
            collective_id=0, has_side_effects=True, vmem_limit_bytes=67_043_328 - 2 * 8 * D - 2 * own * D
        ),
        name="feed_forward",
    )(tokens, w_up, w_down, out_gain.reshape(1, D), out_shift.reshape(1, D))


def solution(mesh):
    sizes = (mesh.shape["rep"], mesh.shape["fs"], mesh.shape["tp"])
    in_specs = (P(("rep", "fs", "tp"), None), P("fs", "tp"), P("tp", "fs"), P(), P())
    out_specs = P(("rep", "fs", "tp"), None)
    return jax.shard_map(
        functools.partial(shards, sizes), mesh=mesh, in_specs=in_specs, out_specs=out_specs, check_vma=False
    )
```
